32 devices in a mesh: st: 16 (over z, y, x), tp: 2 (over core).
Axes of the slice: x: 2, y: 2, z: 4, core: 2. Of those that a mesh axis runs over, the one named last changes fastest.
Arguments:
- tokens: bfloat16 [12288, 2048], P('st'), may hold values from -6 to 6, as said below
- route_ids: int32 [192, 4], P('st'), may hold values from 0 to 383, as said below
- store: bfloat16 [384, 128, 2048], P('st'), may hold values from -6 to 6, as said below
- token_gain: float32 [2048], replicated, may hold values from 0.1 to 1.9
- store_gain: float32 [2048], replicated, may hold values from 0.1 to 1.9
- carry_weight: bfloat16 [2048, 512], P(None, 'tp'), may hold values from -0.125 to 0.125
- spatial_weight: bfloat16 [2048, 512], P(None, 'tp'), may hold values from -0.125 to 0.125
- spatial_gain: float32 [512], P('tp'), may hold values from 0.1 to 1.9
- position_mix: bfloat16 [8, 128, 128], P('tp'), may hold values from -0.5 to 0.5
- position_bias: float32 [8, 128], P('tp'), may hold values from 0.1 to 1.9
- query_weight: bfloat16 [2048, 512], P(None, 'tp'), may hold values from -0.86178639 to 0.86178639, as said below
- key_weight: bfloat16 [2048, 512], P(None, 'tp'), may hold values from -0.86178639 to 0.86178639, as said below
- read_weight: bfloat16 [2048, 512], P(None, 'tp'), may hold values from -0.125 to 0.125
- blend_weight: bfloat16 [2048, 512], P(None, 'tp'), may hold values from -0.125 to 0.125
- output_weight: bfloat16 [512, 2048], replicated, may hold values from -0.25 to 0.25
Outputs:
- mixed: bfloat16 [12288, 2048], P(('st', 'tp'))
The draws below stay inside these ranges and needn't reach their ends.
Inputs may be any that keep to these rules, and one draw needn't show every extreme that they name: `route_ids`: each entry is a passage index; passage p is held by index p // 24 of st. All entries of the spans of one index of st (aligned blocks of 12 rows) are different; they name at most 6 passage held by any one index of st, exactly 6 held by the index before their own (cyclically), and at least one held by the index half the axis away. `tokens`: Activations; in some draws the first token of some spans equals a row of a passage that the span reads. `store`: passage rows. `query_weight`: A projection matrix. `key_weight`: A projection matrix.
All inputs are finite; a program needn't handle non-finite values.
Results may differ from the reference program's by a relative error of at most 0.012.
The reference program's roundings to bfloat16 on the way count: a program that leaves them out, or rounds other values in their place, can miss the bound.
Values may be sent and summed in bfloat16 or wider, within the bound.
No kernel may reach another device: no remote copies, remote signals or barrier semaphores. Data moves between devices by JAX's collectives and lax.ppermute only.
A program may use at most 128 MiB of HBM per device.

```python
import jax
import jax.numpy as jnp
from jax import lax

D = 2048
HEADS = 8
HEAD_DIM = 64
WIDTH = 512
BLOCK = 128
SPAN = 64
PICKS = 4
PASS_ROWS = 128
PASS_DEV = 24
TOK_DEV = 768
TOKENS = 12288
PASSAGES = 384
CAP = 6
N_ST = 16


def store_passage(key, passage):
    passage_key = jax.random.fold_in(jax.random.fold_in(key, 5), passage)
    sample = jax.random.normal(passage_key, (PASS_ROWS, D), jnp.float32)
    return jnp.clip(sample, -6.0, 6.0)


def draw_store(key, part):
    indices = jnp.arange(PASSAGES, dtype=jnp.int32)
    return lax.map(lambda passage: store_passage(key, passage).astype(jnp.bfloat16), indices)


def route_table(key):
    base_key = jax.random.fold_in(key, 3)
    span_dev = TOK_DEV // SPAN
    wanted = span_dev * PICKS
    pool_size = N_ST * CAP
    ranks = jax.random.permutation(jax.random.fold_in(base_key, 0), N_ST)
    heat = 1 + ranks % 4
    slots = jnp.arange(pool_size, dtype=jnp.int32)
    slot_owner = slots // CAP
    slot_copy = slots % CAP

    def reader(index):
        subkeys = jax.random.split(jax.random.fold_in(base_key, index + 1), 3)
        raw_score = jax.random.randint(subkeys[0], (pool_size,), 0, 4096, dtype=jnp.int32)
        score = raw_score * heat[slot_owner] * pool_size + slots
        before = (index + N_ST - 1) % N_ST
        across = (index + N_ST // 2) % N_ST
        forced = (slot_owner == before) | (slot_owner == across) & (slot_copy == 0)
        score = jnp.where(forced, slots - pool_size, score)
        chosen = jnp.argsort(score)[:wanted]
        owner_index = slot_owner[chosen]
        offset = jax.random.randint(subkeys[1], (N_ST,), 0, PASS_DEV, dtype=jnp.int32)
        passage = owner_index * PASS_DEV + (offset[owner_index] + slot_copy[chosen]) % PASS_DEV
        shuffle = jax.random.permutation(subkeys[2], wanted)
        return passage[shuffle].reshape(span_dev, PICKS)
    table = lax.map(reader, jnp.arange(N_ST, dtype=jnp.int32))
    return table.reshape(N_ST * span_dev, PICKS).astype(jnp.int32)


def draw_route_ids(key, part):
    return route_table(key)


def draw_tokens(key, part):
    sample = jnp.clip(jax.random.normal(jax.random.fold_in(key, 9), (TOKENS, D), jnp.float32), -6.0, 6.0)
    return sample.astype(jnp.bfloat16)


def query_key_pair(key):
    base_key = jax.random.fold_in(key, 13)
    first = jnp.clip(jax.random.normal(jax.random.fold_in(base_key, 0), (D, WIDTH), jnp.float32), -6.0, 6.0)
    second = jnp.clip(jax.random.normal(jax.random.fold_in(base_key, 1), (D, WIDTH), jnp.float32), -6.0, 6.0)
    first = first * D ** (-0.5)
    second = second * D ** (-0.5)
    return (first, second)


def draw_query_weight(key, part):
    return query_key_pair(key)[0].astype(jnp.bfloat16)


def draw_key_weight(key, part):
    return query_key_pair(key)[1].astype(jnp.bfloat16)


def level_of(rng, dims, cuts, least, high):
    factor_of, own = 1.0, jax.random.fold_in(rng, 6)
    for position, blocks in cuts:
        heights = jnp.exp(jax.random.uniform(jax.random.fold_in(own, position), (blocks,), jnp.float32, least / len(cuts), high / len(cuts)))
        factor_of = factor_of * jnp.repeat(heights, dims[position] // blocks).reshape([-1 if axis == position else 1 for axis in range(len(dims))])
    return factor_of


def noise(rng, extent, deviation, most, cuts=(), held_as=jnp.bfloat16):
    drawn = jax.random.normal(rng, extent, jnp.float32) * deviation
    if len(cuts) > 0:
        drawn = level_of(rng, extent, cuts, -0.22, 0.18) * drawn
    return jnp.clip(drawn, min=-most, max=most).astype(held_as)


def setup_inputs(seed: int = 0) -> dict:
    streams_of = jax.random.split(jax.random.key(seed), 16)
    tokens = draw_tokens(jax.random.fold_in(streams_of[15], 71), 0)
    route_ids = draw_route_ids(jax.random.fold_in(streams_of[15], 71), 0)
    store = draw_store(jax.random.fold_in(streams_of[15], 71), 0)
    token_gain = jnp.clip(1.0 + 0.18 * jax.random.normal(streams_of[3], (D,), jnp.float32), 0.1, 1.9)
    store_gain = jnp.clip(1.0 + 0.18 * jax.random.normal(streams_of[4], (D,), jnp.float32), 0.1, 1.9)
    carry_weight = noise(streams_of[5], (D, WIDTH), D ** -0.5, 0.125, ((1, 2),))
    spatial_weight = noise(streams_of[6], (D, WIDTH), D ** -0.5, 0.125, ((1, 2),))
    spatial_gain = jnp.clip(1.0 + 0.18 * jax.random.normal(streams_of[7], (WIDTH,), jnp.float32), 0.1, 1.9)
    position_mix = noise(streams_of[8], (HEADS, BLOCK, BLOCK), BLOCK ** -0.5, 0.5, ((0, 2),))
    position_bias = jnp.clip(1.0 + 0.18 * jax.random.normal(streams_of[9], (HEADS, BLOCK), jnp.float32), 0.1, 1.9)
    query_weight = draw_query_weight(jax.random.fold_in(streams_of[15], 71), 0)
    key_weight = draw_key_weight(jax.random.fold_in(streams_of[15], 71), 0)
    read_weight = noise(streams_of[12], (D, WIDTH), D ** -0.5, 0.125, ((1, 2),))
    blend_weight = noise(streams_of[13], (D, WIDTH), D ** -0.5, 0.125, ((1, 2),))
    output_weight = noise(streams_of[14], (WIDTH, D), WIDTH ** -0.5, 0.25)
    return dict(tokens=tokens, route_ids=route_ids, store=store, token_gain=token_gain, store_gain=store_gain, carry_weight=carry_weight, spatial_weight=spatial_weight, spatial_gain=spatial_gain, position_mix=position_mix, position_bias=position_bias, query_weight=query_weight, key_weight=key_weight, read_weight=read_weight, blend_weight=blend_weight, output_weight=output_weight)


norm_eps = 1e-06

def rms_scaled(matrix, gain_vector):
    values = matrix.astype(jnp.float32)
    scaled = values * lax.rsqrt(lax.optimization_barrier(jnp.mean(values * values, axis=-1, keepdims=True)) + norm_eps)
    return (scaled * gain_vector.astype(jnp.float32)).astype(jnp.bfloat16)

def passage_partial(queries, key_rows, value_rows):
    score_scale = queries.shape[-1] ** (-0.5)
    scores = jnp.einsum('bthe,bplhe->bpthl', queries.astype(jnp.float32), key_rows.astype(jnp.float32)) * score_scale
    score_peak = lax.optimization_barrier(jnp.max(scores, axis=-1, keepdims=True))
    weights = jnp.exp(scores - score_peak)
    weight_total = lax.optimization_barrier(jnp.sum(weights, axis=-1))
    rounded = lax.optimization_barrier(weights.astype(jnp.bfloat16)).astype(jnp.float32)
    summed = jnp.einsum('bpthl,bplhe->bpthe', rounded, value_rows.astype(jnp.float32))
    partial_value = (summed / weight_total[..., None]).astype(jnp.bfloat16)
    return (partial_value, score_peak[..., 0] + jnp.log(weight_total))

def merge_partials(partial_value, log_total):
    level_top = lax.optimization_barrier(jnp.max(log_total, axis=1, keepdims=True))
    weights = jnp.exp(log_total - level_top)
    weight_total = lax.optimization_barrier(jnp.sum(weights, axis=1))
    summed = lax.optimization_barrier(jnp.sum(weights[..., None] * partial_value.astype(jnp.float32), axis=1))
    return summed / weight_total[..., None]

def reference(tokens, route_ids, store, token_gain, store_gain, carry_weight, spatial_weight, spatial_gain, position_mix, position_bias, query_weight, key_weight, read_weight, blend_weight, output_weight):
    row_count = tokens.shape[0]
    normed = rms_scaled(tokens, token_gain)
    carry_branch = jnp.dot(normed, carry_weight, preferred_element_type=jnp.float32)
    spatial = jax.nn.gelu(jnp.dot(normed, spatial_weight, preferred_element_type=jnp.float32), approximate=False)
    channel_mean = lax.optimization_barrier(jnp.mean(spatial, axis=-1, keepdims=True))
    channel_spread = lax.optimization_barrier(jnp.mean(spatial * spatial, axis=-1, keepdims=True)) - channel_mean * channel_mean
    spatial_in = ((spatial - channel_mean) * lax.rsqrt(channel_spread + norm_eps) * spatial_gain.astype(jnp.float32)).astype(jnp.bfloat16)
    blocks = spatial_in.reshape(row_count // BLOCK, BLOCK, HEADS, HEAD_DIM)
    mixed_blocks = jnp.einsum('hij,njhc->nihc', position_mix.astype(jnp.float32), blocks.astype(jnp.float32))
    mixed_blocks = mixed_blocks + position_bias.astype(jnp.float32).T[None, :, :, None]
    gated_mix = jax.nn.gelu(carry_branch, approximate=False) * mixed_blocks.reshape(row_count, HEADS * HEAD_DIM)

    def project(passage):
        passage_normed = rms_scaled(passage, store_gain)
        return (jnp.dot(passage_normed, key_weight, preferred_element_type=jnp.float32).astype(jnp.bfloat16), jnp.dot(passage_normed, read_weight, preferred_element_type=jnp.float32).astype(jnp.bfloat16))
    store_keys, store_values = lax.map(project, store)
    store_keys = store_keys.reshape(store.shape[0], PASS_ROWS, HEADS, HEAD_DIM)
    store_values = store_values.reshape(store.shape[0], PASS_ROWS, HEADS, HEAD_DIM)
    queries = jnp.dot(normed, query_weight, preferred_element_type=jnp.float32).astype(jnp.bfloat16)
    queries = queries.reshape(row_count // SPAN, SPAN, HEADS, HEAD_DIM)

    def attend(item):
        span_queries, picked = item
        span_keys = store_keys[picked][None]
        span_values = store_values[picked][None]
        partial_value, log_total = passage_partial(span_queries[None], span_keys, span_values)
        return merge_partials(partial_value, log_total)[0]
    memory = lax.map(attend, (queries, route_ids)).reshape(row_count, HEADS * HEAD_DIM)
    blend_gate = jax.nn.sigmoid(jnp.dot(normed, blend_weight, preferred_element_type=jnp.float32))
    mixed_rows = (gated_mix + blend_gate * memory).astype(jnp.bfloat16)
    return jnp.dot(mixed_rows, output_weight, preferred_element_type=jnp.float32).astype(jnp.bfloat16)
```

```python
import functools

import jax
import jax.numpy as jnp
from jax import lax
from jax.experimental import pallas as pl
from jax.experimental.pallas import tpu as pltpu
from jax.sharding import PartitionSpec as P

norm_eps = 1e-06
LANES = 128
LEVEL_TILE = 16
CHUNKS = 2
f32 = jnp.float32
bf16 = jnp.bfloat16


def params(semantics=None):
    return pltpu.CompilerParams(
        dimension_semantics=semantics, vmem_limit_bytes=56 * 1024 * 1024
    )


def rms_rows(values, gain):
    values = values.astype(f32)
    scale = lax.rsqrt(jnp.mean(values * values, axis=-1, keepdims=True) + norm_eps)
    return (values * scale * gain).astype(bf16)


def query_kernel(
    routes, tokens, gain, weight, normed, place, *rest, chunk_count, capacity, picks, span, held
):
    sent = rest[:chunk_count]
    queries, counts = rest[chunk_count:]
    step = pl.program_id(0)
    block = tokens.shape[0]
    rows = rms_rows(tokens[...], gain[...])
    normed[...] = rows
    start = pl.multiple_of(step * block, block)
    queries[pl.ds(start, block), :] = jnp.dot(
        rows, weight[...], preferred_element_type=f32
    ).astype(bf16)

    @pl.when(step == pl.num_programs(0) - 1)
    def _():
        owners = counts.shape[0]

        def clear(index, carry):
            counts[index] = 0
            return carry

        lax.fori_loop(0, owners, clear, 0)
        part = capacity // chunk_count

        def pack(request, carry):
            owner = lax.div(routes[request], held)
            rank = counts[owner]
            counts[owner] = rank + 1
            place[request] = owner * capacity + rank
            source = pl.multiple_of(lax.div(request, picks) * span, span)
            rows = queries[pl.ds(source, span), :]
            for chunk in range(chunk_count):

                @pl.when(lax.div(rank, part) == chunk)
                def _():
                    target = pl.multiple_of((rank - chunk * part) * span, span)
                    sent[chunk][owner, pl.ds(target, span), :] = rows

            return carry

        lax.fori_loop(0, routes.shape[0], pack, 0)


def store_kernel(store, gain, key_weight, read_weight, keys, values):
    count, length, width = store.shape
    rows = rms_rows(store[...].reshape(count * length, width), gain[...])
    found = jnp.dot(rows, key_weight[...], preferred_element_type=f32)
    keys[...] = found.astype(bf16).reshape(keys.shape)
    read = jnp.dot(rows, read_weight[...], preferred_element_type=f32)
    for index in range(count):
        values[index] = read[index * length : (index + 1) * length].T.astype(bf16)


def attend_kernel(local, queries, keys, values, out, *, part, span, head_dim):
    owners = queries.shape[0]
    width = queries.shape[2]
    pairs = width // LANES
    step = pl.program_id(0)
    scale = head_dim ** (-0.5)
    lane = lax.broadcasted_iota(jnp.int32, (span, LANES), 1)
    low = lane < head_dim
    level_row = lax.broadcasted_iota(jnp.int32, (LEVEL_TILE, LANES), 0)

    def one_owner(owner, carry):
        levels = [jnp.zeros((LEVEL_TILE, LANES), f32) for _ in range(pairs)]
        for slot in range(part):
            held = local[(step * owners + owner) * part + slot]
            for pair in range(pairs):
                cut = slice(pair * LANES, (pair + 1) * LANES)
                piece = queries[owner, slot * span : (slot + 1) * span, cut]
                zero = jnp.zeros_like(piece)
                both = jnp.concatenate(
                    [jnp.where(low, piece, zero), jnp.where(low, zero, piece)], axis=0
                )
                scores = (
                    lax.dot_general(
                        keys[held, :, cut],
                        both,
                        (((1,), (1,)), ((), ())),
                        preferred_element_type=f32,
                    )
                    * scale
                )
                peak = jnp.max(scores, axis=0, keepdims=True)
                weights = jnp.exp(scores - peak)
                total = jnp.sum(weights, axis=0, keepdims=True)
                summed = jnp.dot(
                    values[held, cut, :], weights.astype(bf16), preferred_element_type=f32
                )
                summed = jnp.where(low, summed[:head_dim], summed[head_dim:])
                out[owner, slot * span : (slot + 1) * span, cut] = (summed / total).astype(bf16)
                level = peak + jnp.log(total)
                first = level.astype(bf16).astype(f32)
                second = (level - first).astype(bf16).astype(f32)
                third = level - first - second
                for offset, row in enumerate((first, second, third)):
                    levels[pair] = jnp.where(
                        level_row == 3 * slot + offset, row, levels[pair]
                    )
        for pair in range(pairs):
            cut = slice(pair * LANES, (pair + 1) * LANES)
            out[owner, part * span : part * span + LEVEL_TILE, cut] = levels[pair].astype(bf16)
        return carry

    lax.fori_loop(0, owners, one_owner, 0)


def mixing_kernel(spatial, moments, gain, mix, bias, carry, out, *, head_dim, total_width):
    pairs = spatial.shape[1] // LANES
    mean = moments[:, 0:1] / total_width
    spread = moments[:, 1:2] / total_width - mean * mean
    rows = ((spatial[...] - mean) * lax.rsqrt(spread + norm_eps) * gain[...]).astype(bf16)
    lane = lax.broadcasted_iota(jnp.int32, (spatial.shape[0], LANES), 1)
    for pair in range(pairs):
        cut = slice(pair * LANES, (pair + 1) * LANES)
        first = jnp.dot(mix[2 * pair], rows[:, cut], preferred_element_type=f32)
        second = jnp.dot(mix[2 * pair + 1], rows[:, cut], preferred_element_type=f32)
        first = first + bias[:, 2 * pair : 2 * pair + 1]
        second = second + bias[:, 2 * pair + 1 : 2 * pair + 2]
        out[:, cut] = carry[:, cut] * jnp.where(lane < head_dim, first, second)


def merge_kernel(
    place, core, gated, gate, *rest, chunk_count, capacity, picks, span, head_dim
):
    back = rest[:chunk_count]
    keep, send = rest[chunk_count:]
    part = capacity // chunk_count
    spans = gated.shape[0] // span
    width = gated.shape[1]
    half = spans // 2
    lane = lax.broadcasted_iota(jnp.int32, (span, LANES), 1)
    low = lane < head_dim
    level_row = lax.broadcasted_iota(jnp.int32, (LEVEL_TILE, width), 0)

    def one_span(index, carry):
        levels = []
        pieces = []
        for pick in range(picks):
            at = place[index * picks + pick]
            owner = lax.div(at, capacity)
            rank = lax.rem(at, capacity)
            chunk = lax.div(rank, part)
            slot = rank - chunk * part
            source = pl.multiple_of(slot * span, span)
            piece = back[0][owner, pl.ds(source, span), :]
            tile = back[0][owner, part * span : part * span + LEVEL_TILE, :]
            piece = piece.astype(f32)
            tile = tile.astype(f32)
            for other in range(1, chunk_count):
                here = chunk == other
                piece = jnp.where(
                    here, back[other][owner, pl.ds(source, span), :].astype(f32), piece
                )
                tile = jnp.where(
                    here,
                    back[other][owner, part * span : part * span + LEVEL_TILE, :].astype(f32),
                    tile,
                )
            wanted = (level_row >= 3 * slot) & (level_row < 3 * slot + 3)
            levels.append(jnp.sum(jnp.where(wanted, tile, 0.0), axis=0, keepdims=True))
            pieces.append(piece)
        top = functools.reduce(jnp.maximum, levels)
        weights = [jnp.exp(level - top) for level in levels]
        total = functools.reduce(jnp.add, weights)
        summed = functools.reduce(jnp.add, [w * p for w, p in zip(weights, pieces)])
        memory = summed / total
        stacked = jnp.concatenate([memory[:, :LANES], memory[:, LANES:]], axis=0).T
        upper = stacked[:span]
        lower = stacked[span:]
        first = jnp.where(low, upper, pltpu.roll(lower, head_dim, 1))
        second = jnp.where(low, pltpu.roll(upper, head_dim, 1), lower)
        by_rows = jnp.concatenate([first, second], axis=1)
        start = pl.multiple_of(index * span, span)
        mixed = gated[pl.ds(start, span), :] + gate[pl.ds(start, span), :] * by_rows
        mixed = mixed.astype(bf16)
        side = lax.div(index, half)
        target = pl.multiple_of((index - side * half) * span, span)

        @pl.when(side == core[0])
        def _():
            keep[pl.ds(target, span), :] = mixed

        @pl.when(side != core[0])
        def _():
            send[pl.ds(target, span), :] = mixed

        return carry

    lax.fori_loop(0, spans, one_span, 0)


def output_kernel(core, keep, other, weight, out):
    width = keep.shape[1]
    own = pl.multiple_of(core[0] * width, width)
    far = pl.multiple_of((1 - core[0]) * width, width)
    out[...] = (
        jnp.dot(keep[...], weight[pl.ds(own, width), :], preferred_element_type=f32)
        + jnp.dot(other[...], weight[pl.ds(far, width), :], preferred_element_type=f32)
    ).astype(bf16)


def divisor(count, most):
    return max(size for size in range(1, most + 1) if count % size == 0)


def per_device(
    tokens,
    route_ids,
    store,
    token_gain,
    store_gain,
    carry_weight,
    spatial_weight,
    spatial_gain,
    position_mix,
    position_bias,
    query_weight,
    key_weight,
    read_weight,
    blend_weight,
    output_weight,
):
    row_count, model = tokens.shape
    local_heads, block_length = position_mix.shape[:2]
    width = carry_weight.shape[1]
    head_dim = width // local_heads
    span_count, picks = route_ids.shape
    span = row_count // span_count
    held, length = store.shape[:2]
    owners = lax.axis_size("st")
    cores = lax.axis_size("tp")
    requests = span_count * picks
    capacity = max(1, 2 * requests // owners)
    chunk_count = CHUNKS if capacity % CHUNKS == 0 else 1
    part = capacity // chunk_count
    smem = pl.BlockSpec(memory_space=pltpu.SMEM)
    whole = pl.BlockSpec(memory_space=pltpu.VMEM)
    core = lax.axis_index("tp").astype(jnp.int32).reshape(1)
    flat_ids = route_ids.reshape(requests)

    blocks = 3 if row_count % (3 * 128) == 0 else 1
    token_block = row_count // blocks
    packed = jax.ShapeDtypeStruct((owners, part * span, width), bf16)
    normed, place, *sent = pl.pallas_call(
        functools.partial(
            query_kernel,
            chunk_count=chunk_count,
            capacity=capacity,
            picks=picks,
            span=span,
            held=held,
        ),
        grid=(blocks,),
        in_specs=[
            smem,
            pl.BlockSpec((token_block, model), lambda i: (i, 0)),
            pl.BlockSpec((1, model), lambda i: (0, 0)),
            pl.BlockSpec((model, width), lambda i: (0, 0)),
        ],
        out_specs=[
            pl.BlockSpec((token_block, model), lambda i: (i, 0)),
            smem,
        ]
        + [pl.BlockSpec(packed.shape, lambda i: (0, 0, 0))] * chunk_count,
        out_shape=[
            jax.ShapeDtypeStruct((row_count, model), bf16),
            jax.ShapeDtypeStruct((requests,), jnp.int32),
        ]
        + [packed] * chunk_count,
        scratch_shapes=[
            pltpu.VMEM((row_count, width), bf16),
            pltpu.SMEM((owners,), jnp.int32),
        ],
        compiler_params=params(("arbitrary",)),
        name="queries",
    )(flat_ids, tokens, token_gain.reshape(1, model), query_weight)

    received = [
        lax.all_to_all(piece, "st", split_axis=0, concat_axis=0, tiled=True) for piece in sent
    ]

    all_ids = lax.all_gather(flat_ids, "st", axis=0)
    mine = all_ids // held == lax.axis_index("st")
    order = jnp.arange(requests, dtype=jnp.int32)
    rank = jnp.sum(
        (mine[:, None, :] & (order[None, None, :] < order[None, :, None])).astype(jnp.int32),
        axis=2,
    )
    ranks = jnp.arange(capacity, dtype=jnp.int32)[None, :, None]
    local = jnp.sum(
        jnp.where(mine[:, None, :] & (rank[:, None, :] == ranks), (all_ids % held)[:, None, :], 0),
        axis=2,
    )

    group = divisor(held, 4)
    keys, values = pl.pallas_call(
        store_kernel,
        grid=(held // group,),
        in_specs=[
            pl.BlockSpec((group, length, model), lambda i: (i, 0, 0)),
            pl.BlockSpec((1, model), lambda i: (0, 0)),
            pl.BlockSpec((model, width), lambda i: (0, 0)),
            pl.BlockSpec((model, width), lambda i: (0, 0)),
        ],
        out_specs=[
            pl.BlockSpec((group, length, width), lambda i: (i, 0, 0)),
            pl.BlockSpec((group, width, length), lambda i: (i, 0, 0)),
        ],
        out_shape=[
            jax.ShapeDtypeStruct((held, length, width), bf16),
            jax.ShapeDtypeStruct((held, width, length), bf16),
        ],
        compiler_params=params(("arbitrary",)),
        name="store_rows",
    )(store, store_gain.reshape(1, model), key_weight, read_weight)

    back_rows = part * span + LEVEL_TILE
    owner_group = divisor(owners, 4)
    back = []
    for chunk in range(chunk_count):
        flat_local = local[:, chunk * part : (chunk + 1) * part].reshape(owners * part)
        partial = pl.pallas_call(
            functools.partial(attend_kernel, part=part, span=span, head_dim=head_dim),
            grid=(owners // owner_group,),
            in_specs=[
                smem,
                pl.BlockSpec((owner_group, part * span, width), lambda i: (i, 0, 0)),
                pl.BlockSpec((held, length, width), lambda i: (0, 0, 0)),
                pl.BlockSpec((held, width, length), lambda i: (0, 0, 0)),
            ],
            out_specs=pl.BlockSpec((owner_group, back_rows, width), lambda i: (i, 0, 0)),
            out_shape=jax.ShapeDtypeStruct((owners, back_rows, width), bf16),
            compiler_params=params(("arbitrary",)),
            name="attend",
        )(flat_local, received[chunk], keys, values)
        back.append(lax.all_to_all(partial, "st", split_axis=0, concat_axis=0, tiled=True))

    spatial = jax.nn.gelu(
        jnp.dot(normed, spatial_weight, preferred_element_type=f32), approximate=False
    )
    moments = lax.psum(
        jnp.stack([jnp.sum(spatial, axis=1), jnp.sum(spatial * spatial, axis=1)], axis=1), "tp"
    )
    carry = jax.nn.gelu(
        jnp.dot(normed, carry_weight, preferred_element_type=f32), approximate=False
    )
    gate = jax.nn.sigmoid(jnp.dot(normed, blend_weight, preferred_element_type=f32))
    gated = pl.pallas_call(
        functools.partial(mixing_kernel, head_dim=head_dim, total_width=width * cores),
        grid=(row_count // block_length,),
        in_specs=[
            pl.BlockSpec((block_length, width), lambda i: (i, 0)),
            pl.BlockSpec((block_length, 2), lambda i: (i, 0)),
            pl.BlockSpec((1, width), lambda i: (0, 0)),
            pl.BlockSpec(position_mix.shape, lambda i: (0, 0, 0)),
            pl.BlockSpec((block_length, local_heads), lambda i: (0, 0)),
            pl.BlockSpec((block_length, width), lambda i: (i, 0)),
        ],
        out_specs=pl.BlockSpec((block_length, width), lambda i: (i, 0)),
        out_shape=jax.ShapeDtypeStruct((row_count, width), f32),
        compiler_params=params(("arbitrary",)),
        name="mixing",
    )(spatial, moments, spatial_gain.reshape(1, width), position_mix, position_bias.T, carry)

    half = jax.ShapeDtypeStruct((row_count // cores, width), bf16)
    keep, send = pl.pallas_call(
        functools.partial(
            merge_kernel,
            chunk_count=chunk_count,
            capacity=capacity,
            picks=picks,
            span=span,
            head_dim=head_dim,
        ),
        in_specs=[smem, smem, whole, whole] + [whole] * chunk_count,
        out_specs=[whole, whole],
        out_shape=[half, half],
        compiler_params=params(),
        name="merge",
    )(place, core, gated, gate, *back)
    other = lax.ppermute(send, "tp", [(0, 1), (1, 0)])
    column = model // 4
    return pl.pallas_call(
        output_kernel,
        grid=(4,),
        in_specs=[
            smem,
            pl.BlockSpec(half.shape, lambda i: (0, 0)),
            pl.BlockSpec(half.shape, lambda i: (0, 0)),
            pl.BlockSpec((width * cores, column), lambda i: (0, i)),
        ],
        out_specs=pl.BlockSpec((row_count // cores, column), lambda i: (0, i)),
        out_shape=jax.ShapeDtypeStruct((row_count // cores, model), bf16),
        compiler_params=params(("arbitrary",)),
        name="project",
    )(core, keep, other, output_weight)


def solution(mesh):
    in_specs = (
        P("st", None),
        P("st", None),
        P("st", None, None),
        P(),
        P(),
        P(None, "tp"),
        P(None, "tp"),
        P("tp"),
        P("tp", None, None),
        P("tp", None),
        P(None, "tp"),
        P(None, "tp"),
        P(None, "tp"),
        P(None, "tp"),
        P(),
    )
    out_specs = P(("st", "tp"), None)
    return jax.shard_map(
        per_device, mesh=mesh, in_specs=in_specs, out_specs=out_specs, check_vma=False
    )
```

```python
import functools

import jax
import jax.numpy as jnp
from jax import lax
from jax.experimental import pallas as pl
from jax.experimental.pallas import tpu as pltpu
from jax.sharding import PartitionSpec as P

norm_eps = 1e-06
LANES = 128
LEVEL_TILE = 16
CHUNKS = 2
f32 = jnp.float32
bf16 = jnp.bfloat16


def params(semantics=None):
    return pltpu.CompilerParams(
        dimension_semantics=semantics, vmem_limit_bytes=56 * 1024 * 1024
    )


def rms_rows(values, gain):
    values = values.astype(f32)
    scale = lax.rsqrt(jnp.mean(values * values, axis=-1, keepdims=True) + norm_eps)
    return (values * scale * gain).astype(bf16)


def query_kernel(
    routes, slots, tokens, gain, weight, normed, place, local, *rest, chunk_count, capacity, picks, span, held
):
    sent = rest[:chunk_count]
    queries, counts = rest[chunk_count:]
    step = pl.program_id(0)
    block = tokens.shape[0]
    rows = rms_rows(tokens[...], gain[...])
    normed[...] = rows
    start = pl.multiple_of(step * block, block)
    queries[pl.ds(start, block), :] = jnp.dot(
        rows, weight[...], preferred_element_type=f32
    ).astype(bf16)

    @pl.when(step == pl.num_programs(0) - 1)
    def _():
        owners = counts.shape[0]

        def clear(index, carry):
            counts[index] = 0
            for rank in range(capacity):
                local[rank, index] = slots[rank, index]
            return carry

        lax.fori_loop(0, owners, clear, 0)
        part = capacity // chunk_count

        def pack(request, carry):
            owner = lax.div(routes[request], held)
            rank = counts[owner]
            counts[owner] = rank + 1
            place[request] = owner * capacity + rank
            source = pl.multiple_of(lax.div(request, picks) * span, span)
            rows = queries[pl.ds(source, span), :]
            for chunk in range(chunk_count):

                @pl.when(lax.div(rank, part) == chunk)
                def _():
                    target = pl.multiple_of((rank - chunk * part) * span, span)
                    sent[chunk][owner, pl.ds(target, span), :] = rows

            return carry

        lax.fori_loop(0, routes.shape[0], pack, 0)


def store_kernel(store, gain, key_weight, read_weight, keys, values):
    count, length, width = store.shape
    rows = rms_rows(store[...].reshape(count * length, width), gain[...])
    found = jnp.dot(rows, key_weight[...], preferred_element_type=f32)
    keys[...] = found.astype(bf16).reshape(keys.shape)
    read = jnp.dot(rows, read_weight[...], preferred_element_type=f32)
    for index in range(count):
        values[index] = read[index * length : (index + 1) * length].T.astype(bf16)


def attend_kernel(local, queries, keys, values, out, *, base, part, span, head_dim):
    owners = queries.shape[0]
    width = queries.shape[2]
    pairs = width // LANES
    step = pl.program_id(0)
    scale = head_dim ** (-0.5)
    lane = lax.broadcasted_iota(jnp.int32, (span, LANES), 1)
    low = lane < head_dim
    level_row = lax.broadcasted_iota(jnp.int32, (LEVEL_TILE, LANES), 0)

    def one_owner(owner, carry):
        levels = [jnp.zeros((LEVEL_TILE, LANES), f32) for _ in range(pairs)]
        for slot in range(part):
            held = local[base + slot, step * owners + owner]
            for pair in range(pairs):
                cut = slice(pair * LANES, (pair + 1) * LANES)
                piece = queries[owner, slot * span : (slot + 1) * span, cut]
                zero = jnp.zeros_like(piece)
                both = jnp.concatenate(
                    [jnp.where(low, piece, zero), jnp.where(low, zero, piece)], axis=0
                )
                scores = (
                    lax.dot_general(
                        keys[held, :, cut],
                        both,
                        (((1,), (1,)), ((), ())),
                        preferred_element_type=f32,
                    )
                    * scale
                )
                peak = jnp.max(scores, axis=0, keepdims=True)
                weights = jnp.exp(scores - peak)
                total = jnp.sum(weights, axis=0, keepdims=True)
                summed = jnp.dot(
                    values[held, cut, :], weights.astype(bf16), preferred_element_type=f32
                )
                summed = jnp.where(low, summed[:head_dim], summed[head_dim:])
                out[owner, slot * span : (slot + 1) * span, cut] = (summed / total).astype(bf16)
                level = peak + jnp.log(total)
                first = level.astype(bf16).astype(f32)
                second = (level - first).astype(bf16).astype(f32)
                third = level - first - second
                for offset, row in enumerate((first, second, third)):
                    levels[pair] = jnp.where(
                        level_row == 3 * slot + offset, row, levels[pair]
                    )
        for pair in range(pairs):
            cut = slice(pair * LANES, (pair + 1) * LANES)
            out[owner, part * span : part * span + LEVEL_TILE, cut] = levels[pair].astype(bf16)
        return carry

    lax.fori_loop(0, owners, one_owner, 0)


def mixing_kernel(spatial, moments, gain, mix, bias, carry, out, *, head_dim, total_width):
    pairs = spatial.shape[1] // LANES
    mean = moments[:, 0:1] / total_width
    spread = moments[:, 1:2] / total_width - mean * mean
    rows = ((spatial[...] - mean) * lax.rsqrt(spread + norm_eps) * gain[...]).astype(bf16)
    lane = lax.broadcasted_iota(jnp.int32, (spatial.shape[0], LANES), 1)
    for pair in range(pairs):
        cut = slice(pair * LANES, (pair + 1) * LANES)
        first = jnp.dot(mix[2 * pair], rows[:, cut], preferred_element_type=f32)
        second = jnp.dot(mix[2 * pair + 1], rows[:, cut], preferred_element_type=f32)
        first = first + bias[:, 2 * pair : 2 * pair + 1]
        second = second + bias[:, 2 * pair + 1 : 2 * pair + 2]
        out[:, cut] = carry[:, cut] * jnp.where(lane < head_dim, first, second)


def merge_kernel(
    place, core, gated, gate, *rest, chunk_count, capacity, picks, span, head_dim
):
    back = rest[:chunk_count]
    keep, send = rest[chunk_count:]
    part = capacity // chunk_count
    spans = gated.shape[0] // span
    width = gated.shape[1]
    half = spans // 2
    lane = lax.broadcasted_iota(jnp.int32, (span, LANES), 1)
    low = lane < head_dim
    level_row = lax.broadcasted_iota(jnp.int32, (LEVEL_TILE, width), 0)

    def one_span(index, carry):
        levels = []
        pieces = []
        for pick in range(picks):
            at = place[index * picks + pick]
            owner = lax.div(at, capacity)
            rank = lax.rem(at, capacity)
            chunk = lax.div(rank, part)
            slot = rank - chunk * part
            source = pl.multiple_of(slot * span, span)
            piece = back[0][owner, pl.ds(source, span), :]
            tile = back[0][owner, part * span : part * span + LEVEL_TILE, :]
            piece = piece.astype(f32)
            tile = tile.astype(f32)
            for other in range(1, chunk_count):
                here = chunk == other
                piece = jnp.where(
                    here, back[other][owner, pl.ds(source, span), :].astype(f32), piece
                )
                tile = jnp.where(
                    here,
                    back[other][owner, part * span : part * span + LEVEL_TILE, :].astype(f32),
                    tile,
                )
            wanted = (level_row >= 3 * slot) & (level_row < 3 * slot + 3)
            levels.append(jnp.sum(jnp.where(wanted, tile, 0.0), axis=0, keepdims=True))
            pieces.append(piece)
        top = functools.reduce(jnp.maximum, levels)
        weights = [jnp.exp(level - top) for level in levels]
        total = functools.reduce(jnp.add, weights)
        summed = functools.reduce(jnp.add, [w * p for w, p in zip(weights, pieces)])
        memory = summed / total
        stacked = jnp.concatenate([memory[:, :LANES], memory[:, LANES:]], axis=0).T
        upper = stacked[:span]
        lower = stacked[span:]
        first = jnp.where(low, upper, pltpu.roll(lower, head_dim, 1))
        second = jnp.where(low, pltpu.roll(upper, head_dim, 1), lower)
        by_rows = jnp.concatenate([first, second], axis=1)
        start = pl.multiple_of(index * span, span)
        mixed = gated[pl.ds(start, span), :] + gate[pl.ds(start, span), :] * by_rows
        mixed = mixed.astype(bf16)
        side = lax.div(index, half)
        target = pl.multiple_of((index - side * half) * span, span)

        @pl.when(side == core[0])
        def _():
            keep[pl.ds(target, span), :] = mixed

        @pl.when(side != core[0])
        def _():
            send[pl.ds(target, span), :] = mixed

        return carry

    lax.fori_loop(0, spans, one_span, 0)


def output_kernel(core, keep, other, weight, out):
    width = keep.shape[1]
    own = pl.multiple_of(core[0] * width, width)
    far = pl.multiple_of((1 - core[0]) * width, width)
    out[...] = (
        jnp.dot(keep[...], weight[pl.ds(own, width), :], preferred_element_type=f32)
        + jnp.dot(other[...], weight[pl.ds(far, width), :], preferred_element_type=f32)
    ).astype(bf16)


def divisor(count, most):
    return max(size for size in range(1, most + 1) if count % size == 0)


def per_device(
    tokens,
    route_ids,
    store,
    token_gain,
    store_gain,
    carry_weight,
    spatial_weight,
    spatial_gain,
    position_mix,
    position_bias,
    query_weight,
    key_weight,
    read_weight,
    blend_weight,
    output_weight,
):
    row_count, model = tokens.shape
    local_heads, block_length = position_mix.shape[:2]
    width = carry_weight.shape[1]
    head_dim = width // local_heads
    span_count, picks = route_ids.shape
    span = row_count // span_count
    held, length = store.shape[:2]
    owners = lax.axis_size("st")
    cores = lax.axis_size("tp")
    requests = span_count * picks
    capacity = max(1, 2 * requests // owners)
    chunk_count = CHUNKS if capacity % CHUNKS == 0 else 1
    part = capacity // chunk_count
    smem = pl.BlockSpec(memory_space=pltpu.SMEM)
    whole = pl.BlockSpec(memory_space=pltpu.VMEM)
    core = lax.axis_index("tp").astype(jnp.int32).reshape(1)
    flat_ids = route_ids.reshape(requests)

    all_ids = lax.all_gather(flat_ids, "st", axis=0)
    mine = all_ids // held == lax.axis_index("st")
    order = jnp.arange(requests, dtype=jnp.int32)
    rank = jnp.sum(
        (mine[:, None, :] & (order[None, None, :] < order[None, :, None])).astype(jnp.int32),
        axis=2,
    )
    ranks = jnp.arange(capacity, dtype=jnp.int32)[:, None, None]
    local = jnp.sum(
        jnp.where(mine[None] & (rank[None] == ranks), (all_ids % held)[None], 0), axis=2
    )

    blocks = 3 if row_count % (3 * 128) == 0 else 1
    token_block = row_count // blocks
    packed = jax.ShapeDtypeStruct((owners, part * span, width), bf16)
    normed, place, local, *sent = pl.pallas_call(
        functools.partial(
            query_kernel,
            chunk_count=chunk_count,
            capacity=capacity,
            picks=picks,
            span=span,
            held=held,
        ),
        grid=(blocks,),
        in_specs=[
            smem,
            smem,
            pl.BlockSpec((token_block, model), lambda i: (i, 0)),
            pl.BlockSpec((1, model), lambda i: (0, 0)),
            pl.BlockSpec((model, width), lambda i: (0, 0)),
        ],
        out_specs=[
            pl.BlockSpec((token_block, model), lambda i: (i, 0)),
            smem,
            smem,
        ]
        + [pl.BlockSpec(packed.shape, lambda i: (0, 0, 0))] * chunk_count,
        out_shape=[
            jax.ShapeDtypeStruct((row_count, model), bf16),
            jax.ShapeDtypeStruct((requests,), jnp.int32),
            jax.ShapeDtypeStruct((capacity, owners), jnp.int32),
        ]
        + [packed] * chunk_count,
        scratch_shapes=[
            pltpu.VMEM((row_count, width), bf16),
            pltpu.SMEM((owners,), jnp.int32),
        ],
        compiler_params=params(("arbitrary",)),
        name="queries",
    )(flat_ids, local, tokens, token_gain.reshape(1, model), query_weight)

    received = [lax.all_to_all(sent[0], "st", split_axis=0, concat_axis=0, tiled=True)]

    group = divisor(held, 4)
    keys, values = pl.pallas_call(
        store_kernel,
        grid=(held // group,),
        in_specs=[
            pl.BlockSpec((group, length, model), lambda i: (i, 0, 0)),
            pl.BlockSpec((1, model), lambda i: (0, 0)),
            pl.BlockSpec((model, width), lambda i: (0, 0)),
            pl.BlockSpec((model, width), lambda i: (0, 0)),
        ],
        out_specs=[
            pl.BlockSpec((group, length, width), lambda i: (i, 0, 0)),
            pl.BlockSpec((group, width, length), lambda i: (i, 0, 0)),
        ],
        out_shape=[
            jax.ShapeDtypeStruct((held, length, width), bf16),
            jax.ShapeDtypeStruct((held, width, length), bf16),
        ],
        compiler_params=params(("arbitrary",)),
        name="store_rows",
    )(store, store_gain.reshape(1, model), key_weight, read_weight)

    spatial = jax.nn.gelu(
        jnp.dot(normed, spatial_weight, preferred_element_type=f32), approximate=False
    )
    moments = lax.psum(
        jnp.stack([jnp.sum(spatial, axis=1), jnp.sum(spatial * spatial, axis=1)], axis=1), "tp"
    )
    carry = jax.nn.gelu(
        jnp.dot(normed, carry_weight, preferred_element_type=f32), approximate=False
    )
    gate = jax.nn.sigmoid(jnp.dot(normed, blend_weight, preferred_element_type=f32))
    gated = pl.pallas_call(
        functools.partial(mixing_kernel, head_dim=head_dim, total_width=width * cores),
        grid=(row_count // block_length,),
        in_specs=[
            pl.BlockSpec((block_length, width), lambda i: (i, 0)),
            pl.BlockSpec((block_length, 2), lambda i: (i, 0)),
            pl.BlockSpec((1, width), lambda i: (0, 0)),
            pl.BlockSpec(position_mix.shape, lambda i: (0, 0, 0)),
            pl.BlockSpec((block_length, local_heads), lambda i: (0, 0)),
            pl.BlockSpec((block_length, width), lambda i: (i, 0)),
        ],
        out_specs=pl.BlockSpec((block_length, width), lambda i: (i, 0)),
        out_shape=jax.ShapeDtypeStruct((row_count, width), f32),
        compiler_params=params(("arbitrary",)),
        name="mixing",
    )(spatial, moments, spatial_gain.reshape(1, width), position_mix, position_bias.T, carry)

    for chunk in range(1, chunk_count):
        received.append(lax.all_to_all(sent[chunk], "st", split_axis=0, concat_axis=0, tiled=True))

    back_rows = part * span + LEVEL_TILE
    owner_group = divisor(owners, 4)
    back = []
    for chunk in range(chunk_count):
        partial = pl.pallas_call(
            functools.partial(
                attend_kernel, base=chunk * part, part=part, span=span, head_dim=head_dim),
            grid=(owners // owner_group,),
            in_specs=[
                smem,
                pl.BlockSpec((owner_group, part * span, width), lambda i: (i, 0, 0)),
                pl.BlockSpec((held, length, width), lambda i: (0, 0, 0)),
                pl.BlockSpec((held, width, length), lambda i: (0, 0, 0)),
            ],
            out_specs=pl.BlockSpec((owner_group, back_rows, width), lambda i: (i, 0, 0)),
            out_shape=jax.ShapeDtypeStruct((owners, back_rows, width), bf16),
            compiler_params=params(("arbitrary",)),
        )(local, received[chunk], keys, values)
        back.append(lax.all_to_all(partial, "st", split_axis=0, concat_axis=0, tiled=True))

    half = jax.ShapeDtypeStruct((row_count // cores, width), bf16)
    keep, send = pl.pallas_call(
        functools.partial(
            merge_kernel,
            chunk_count=chunk_count,
            capacity=capacity,
            picks=picks,
            span=span,
            head_dim=head_dim,
        ),
        in_specs=[smem, smem, whole, whole] + [whole] * chunk_count,
        out_specs=[whole, whole],
        out_shape=[half, half],
        compiler_params=params(),
        name="merge",
    )(place, core, gated, gate, *back)
    other = lax.ppermute(send, "tp", [(0, 1), (1, 0)])
    column = model // 4
    return pl.pallas_call(
        output_kernel,
        grid=(4,),
        in_specs=[
            smem,
            pl.BlockSpec(half.shape, lambda i: (0, 0)),
            pl.BlockSpec(half.shape, lambda i: (0, 0)),
            pl.BlockSpec((width * cores, column), lambda i: (0, i)),
        ],
        out_specs=pl.BlockSpec((row_count // cores, column), lambda i: (0, i)),
        out_shape=jax.ShapeDtypeStruct((row_count // cores, model), bf16),
        compiler_params=params(("arbitrary",)),
        name="project",
    )(core, keep, other, output_weight)


def solution(mesh):
    in_specs = (
        P("st", None),
        P("st", None),
        P("st", None, None),
        P(),
        P(),
        P(None, "tp"),
        P(None, "tp"),
        P("tp"),
        P("tp", None, None),
        P("tp", None),
        P(None, "tp"),
        P(None, "tp"),
        P(None, "tp"),
        P(None, "tp"),
        P(),
    )
    out_specs = P(("st", "tp"), None)

    return jax.shard_map(
        per_device, mesh=mesh, in_specs=in_specs, out_specs=out_specs, check_vma=False
    )
```

```python
import functools

import jax
import jax.numpy as jnp
from jax import lax
from jax.experimental import pallas as pl
from jax.experimental.pallas import tpu as pltpu
from jax.sharding import PartitionSpec as P

norm_eps = 1e-06
LANES = 128
LEVEL_TILE = 16
CHUNKS = 2
f32 = jnp.float32
bf16 = jnp.bfloat16


def params(semantics=None):
    return pltpu.CompilerParams(
        dimension_semantics=semantics, vmem_limit_bytes=56 * 1024 * 1024
    )


def rms_rows(values, gain):
    values = values.astype(f32)
    scale = lax.rsqrt(jnp.mean(values * values, axis=-1, keepdims=True) + norm_eps)
    return (values * scale * gain).astype(bf16)


def query_kernel(
    routes, tokens, gain, weight, normed, place, *rest, chunk_count, capacity, picks, span, held
):
    sent = rest[:chunk_count]
    queries, counts = rest[chunk_count:]
    step = pl.program_id(0)
    block = tokens.shape[0]
    rows = rms_rows(tokens[...], gain[...])
    normed[...] = rows
    start = pl.multiple_of(step * block, block)
    queries[pl.ds(start, block), :] = jnp.dot(
        rows, weight[...], preferred_element_type=f32
    ).astype(bf16)

    @pl.when(step == pl.num_programs(0) - 1)
    def _():
        owners = counts.shape[0]

        def clear(index, carry):
            counts[index] = 0
            return carry

        lax.fori_loop(0, owners, clear, 0)
        part = capacity // chunk_count

        def pack(request, carry):
            owner = lax.div(routes[request], held)
            rank = counts[owner]
            counts[owner] = rank + 1
            place[request] = owner * capacity + rank
            source = pl.multiple_of(lax.div(request, picks) * span, span)
            rows = queries[pl.ds(source, span), :]
            for chunk in range(chunk_count):

                @pl.when(lax.div(rank, part) == chunk)
                def _():
                    target = pl.multiple_of((rank - chunk * part) * span, span)
                    sent[chunk][owner, pl.ds(target, span), :] = rows

            return carry

        lax.fori_loop(0, routes.shape[0], pack, 0)


def store_kernel(store, gain, key_weight, read_weight, keys, values):
    count, length, width = store.shape
    rows = rms_rows(store[...].reshape(count * length, width), gain[...])
    found = jnp.dot(rows, key_weight[...], preferred_element_type=f32)
    keys[...] = found.astype(bf16).reshape(keys.shape)
    read = jnp.dot(rows, read_weight[...], preferred_element_type=f32)
    for index in range(count):
        values[index] = read[index * length : (index + 1) * length].T.astype(bf16)


def attend_kernel(local, queries, keys, values, out, *, base, part, span, head_dim):
    owners = queries.shape[0]
    width = queries.shape[2]
    pairs = width // LANES
    step = pl.program_id(0)
    scale = head_dim ** (-0.5)
    lane = lax.broadcasted_iota(jnp.int32, (span, LANES), 1)
    low = lane < head_dim
    level_row = lax.broadcasted_iota(jnp.int32, (LEVEL_TILE, LANES), 0)

    def one_owner(owner, carry):
        levels = [jnp.zeros((LEVEL_TILE, LANES), f32) for _ in range(pairs)]
        for slot in range(part):
            held = local[base + slot, step * owners + owner]
            for pair in range(pairs):
                cut = slice(pair * LANES, (pair + 1) * LANES)
                piece = queries[owner, slot * span : (slot + 1) * span, cut]
                zero = jnp.zeros_like(piece)
                both = jnp.concatenate(
                    [jnp.where(low, piece, zero), jnp.where(low, zero, piece)], axis=0
                )
                scores = (
                    lax.dot_general(
                        keys[held, :, cut],
                        both,
                        (((1,), (1,)), ((), ())),
                        preferred_element_type=f32,
                    )
                    * scale
                )
                peak = jnp.max(scores, axis=0, keepdims=True)
                weights = jnp.exp(scores - peak)
                total = jnp.sum(weights, axis=0, keepdims=True)
                summed = jnp.dot(
                    values[held, cut, :], weights.astype(bf16), preferred_element_type=f32
                )
                summed = jnp.where(low, summed[:head_dim], summed[head_dim:])
                out[owner, slot * span : (slot + 1) * span, cut] = (summed / total).astype(bf16)
                level = peak + jnp.log(total)
                first = level.astype(bf16).astype(f32)
                second = (level - first).astype(bf16).astype(f32)
                third = level - first - second
                for offset, row in enumerate((first, second, third)):
                    levels[pair] = jnp.where(
                        level_row == 3 * slot + offset, row, levels[pair]
                    )
        for pair in range(pairs):
            cut = slice(pair * LANES, (pair + 1) * LANES)
            out[owner, part * span : part * span + LEVEL_TILE, cut] = levels[pair].astype(bf16)
        return carry

    lax.fori_loop(0, owners, one_owner, 0)


def mixing_kernel(spatial, moments, gain, mix, bias, carry, out, *, head_dim, total_width):
    pairs = spatial.shape[1] // LANES
    mean = moments[:, 0:1] / total_width
    spread = moments[:, 1:2] / total_width - mean * mean
    rows = ((spatial[...] - mean) * lax.rsqrt(spread + norm_eps) * gain[...]).astype(bf16)
    lane = lax.broadcasted_iota(jnp.int32, (spatial.shape[0], LANES), 1)
    for pair in range(pairs):
        cut = slice(pair * LANES, (pair + 1) * LANES)
        first = jnp.dot(mix[2 * pair], rows[:, cut], preferred_element_type=f32)
        second = jnp.dot(mix[2 * pair + 1], rows[:, cut], preferred_element_type=f32)
        first = first + bias[:, 2 * pair : 2 * pair + 1]
        second = second + bias[:, 2 * pair + 1 : 2 * pair + 2]
        out[:, cut] = carry[:, cut] * jnp.where(lane < head_dim, first, second)


def merge_kernel(
    place, core, gated, gate, *rest, chunk_count, capacity, picks, span, head_dim
):
    back = rest[:chunk_count]
    keep, send = rest[chunk_count:]
    part = capacity // chunk_count
    spans = gated.shape[0] // span
    width = gated.shape[1]
    half = spans // 2
    lane = lax.broadcasted_iota(jnp.int32, (span, LANES), 1)
    low = lane < head_dim
    level_row = lax.broadcasted_iota(jnp.int32, (LEVEL_TILE, width), 0)

    def one_span(index, carry):
        levels = []
        pieces = []
        for pick in range(picks):
            at = place[index * picks + pick]
            owner = lax.div(at, capacity)
            rank = lax.rem(at, capacity)
            chunk = lax.div(rank, part)
            slot = rank - chunk * part
            source = pl.multiple_of(slot * span, span)
            piece = back[0][owner, pl.ds(source, span), :]
            tile = back[0][owner, part * span : part * span + LEVEL_TILE, :]
            piece = piece.astype(f32)
            tile = tile.astype(f32)
            for other in range(1, chunk_count):
                here = chunk == other
                piece = jnp.where(
                    here, back[other][owner, pl.ds(source, span), :].astype(f32), piece
                )
                tile = jnp.where(
                    here,
                    back[other][owner, part * span : part * span + LEVEL_TILE, :].astype(f32),
                    tile,
                )
            wanted = (level_row >= 3 * slot) & (level_row < 3 * slot + 3)
            levels.append(jnp.sum(jnp.where(wanted, tile, 0.0), axis=0, keepdims=True))
            pieces.append(piece)
        top = functools.reduce(jnp.maximum, levels)
        weights = [jnp.exp(level - top) for level in levels]
        total = functools.reduce(jnp.add, weights)
        summed = functools.reduce(jnp.add, [w * p for w, p in zip(weights, pieces)])
        memory = summed / total
        stacked = jnp.concatenate([memory[:, :LANES], memory[:, LANES:]], axis=0).T
        upper = stacked[:span]
        lower = stacked[span:]
        first = jnp.where(low, upper, pltpu.roll(lower, head_dim, 1))
        second = jnp.where(low, pltpu.roll(upper, head_dim, 1), lower)
        by_rows = jnp.concatenate([first, second], axis=1)
        start = pl.multiple_of(index * span, span)
        mixed = gated[pl.ds(start, span), :] + gate[pl.ds(start, span), :] * by_rows
        mixed = mixed.astype(bf16)
        side = lax.div(index, half)
        target = pl.multiple_of((index - side * half) * span, span)

        @pl.when(side == core[0])
        def _():
            keep[pl.ds(target, span), :] = mixed

        @pl.when(side != core[0])
        def _():
            send[pl.ds(target, span), :] = mixed

        return carry

    lax.fori_loop(0, spans, one_span, 0)


def output_kernel(core, keep, other, weight, out):
    width = keep.shape[1]
    own = pl.multiple_of(core[0] * width, width)
    far = pl.multiple_of((1 - core[0]) * width, width)
    out[...] = (
        jnp.dot(keep[...], weight[pl.ds(own, width), :], preferred_element_type=f32)
        + jnp.dot(other[...], weight[pl.ds(far, width), :], preferred_element_type=f32)
    ).astype(bf16)


def divisor(count, most):
    return max(size for size in range(1, most + 1) if count % size == 0)


def per_device(
    tokens,
    route_ids,
    store,
    token_gain,
    store_gain,
    carry_weight,
    spatial_weight,
    spatial_gain,
    position_mix,
    position_bias,
    query_weight,
    key_weight,
    read_weight,
    blend_weight,
    output_weight,
):
    row_count, model = tokens.shape
    local_heads, block_length = position_mix.shape[:2]
    width = carry_weight.shape[1]
    head_dim = width // local_heads
    span_count, picks = route_ids.shape
    span = row_count // span_count
    held, length = store.shape[:2]
    owners = lax.axis_size("st")
    cores = lax.axis_size("tp")
    requests = span_count * picks
    capacity = max(1, 2 * requests // owners)
    chunk_count = CHUNKS if capacity % CHUNKS == 0 else 1
    part = capacity // chunk_count
    smem = pl.BlockSpec(memory_space=pltpu.SMEM)
    whole = pl.BlockSpec(memory_space=pltpu.VMEM)
    core = lax.axis_index("tp").astype(jnp.int32).reshape(1)
    flat_ids = route_ids.reshape(requests)

    all_ids = lax.all_to_all(
        jnp.broadcast_to(flat_ids[None, :], (owners, requests)),
        "st",
        split_axis=0,
        concat_axis=0,
        tiled=True,
    )
    mine = all_ids // held == lax.axis_index("st")
    order = jnp.arange(requests, dtype=jnp.int32)
    rank = jnp.sum(
        (mine[:, None, :] & (order[None, None, :] < order[None, :, None])).astype(jnp.int32),
        axis=2,
    )
    ranks = jnp.arange(capacity, dtype=jnp.int32)[:, None, None]
    local = jnp.sum(
        jnp.where(mine[None] & (rank[None] == ranks), (all_ids % held)[None], 0), axis=2
    )

    blocks = 3 if row_count % (3 * 128) == 0 else 1
    token_block = row_count // blocks
    packed = jax.ShapeDtypeStruct((owners, part * span, width), bf16)
    normed, place, *sent = pl.pallas_call(
        functools.partial(
            query_kernel,
            chunk_count=chunk_count,
            capacity=capacity,
            picks=picks,
            span=span,
            held=held,
        ),
        grid=(blocks,),
        in_specs=[
            smem,
            pl.BlockSpec((token_block, model), lambda i: (i, 0)),
            pl.BlockSpec((1, model), lambda i: (0, 0)),
            pl.BlockSpec((model, width), lambda i: (0, 0)),
        ],
        out_specs=[
            pl.BlockSpec((token_block, model), lambda i: (i, 0)),
            smem,
        ]
        + [pl.BlockSpec(packed.shape, lambda i: (0, 0, 0))] * chunk_count,
        out_shape=[
            jax.ShapeDtypeStruct((row_count, model), bf16),
            jax.ShapeDtypeStruct((requests,), jnp.int32),
        ]
        + [packed] * chunk_count,
        scratch_shapes=[
            pltpu.VMEM((row_count, width), bf16),
            pltpu.SMEM((owners,), jnp.int32),
        ],
        compiler_params=params(("arbitrary",)),
        name="queries",
    )(flat_ids, tokens, token_gain.reshape(1, model), query_weight)

    received = [lax.all_to_all(sent[0], "st", split_axis=0, concat_axis=0, tiled=True)]

    group = divisor(held, 4)
    keys, values = pl.pallas_call(
        store_kernel,
        grid=(held // group,),
        in_specs=[
            pl.BlockSpec((group, length, model), lambda i: (i, 0, 0)),
            pl.BlockSpec((1, model), lambda i: (0, 0)),
            pl.BlockSpec((model, width), lambda i: (0, 0)),
            pl.BlockSpec((model, width), lambda i: (0, 0)),
        ],
        out_specs=[
            pl.BlockSpec((group, length, width), lambda i: (i, 0, 0)),
            pl.BlockSpec((group, width, length), lambda i: (i, 0, 0)),
        ],
        out_shape=[
            jax.ShapeDtypeStruct((held, length, width), bf16),
            jax.ShapeDtypeStruct((held, width, length), bf16),
        ],
        compiler_params=params(("arbitrary",)),
        name="store_rows",
    )(store, store_gain.reshape(1, model), key_weight, read_weight)

    spatial = jax.nn.gelu(
        jnp.dot(normed, spatial_weight, preferred_element_type=f32), approximate=False
    )
    moments = lax.psum(
        jnp.stack([jnp.sum(spatial, axis=1), jnp.sum(spatial * spatial, axis=1)], axis=1), "tp"
    )
    carry = jax.nn.gelu(
        jnp.dot(normed, carry_weight, preferred_element_type=f32), approximate=False
    )
    gate = jax.nn.sigmoid(jnp.dot(normed, blend_weight, preferred_element_type=f32))
    gated = pl.pallas_call(
        functools.partial(mixing_kernel, head_dim=head_dim, total_width=width * cores),
        grid=(row_count // block_length,),
        in_specs=[
            pl.BlockSpec((block_length, width), lambda i: (i, 0)),
            pl.BlockSpec((block_length, 2), lambda i: (i, 0)),
            pl.BlockSpec((1, width), lambda i: (0, 0)),
            pl.BlockSpec(position_mix.shape, lambda i: (0, 0, 0)),
            pl.BlockSpec((block_length, local_heads), lambda i: (0, 0)),
            pl.BlockSpec((block_length, width), lambda i: (i, 0)),
        ],
        out_specs=pl.BlockSpec((block_length, width), lambda i: (i, 0)),
        out_shape=jax.ShapeDtypeStruct((row_count, width), f32),
        compiler_params=params(("arbitrary",)),
        name="mixing",
    )(spatial, moments, spatial_gain.reshape(1, width), position_mix, position_bias.T, carry)

    for chunk in range(1, chunk_count):
        received.append(lax.all_to_all(sent[chunk], "st", split_axis=0, concat_axis=0, tiled=True))

    back_rows = part * span + LEVEL_TILE
    owner_group = divisor(owners, 4)
    back = []
    for chunk in range(chunk_count):
        partial = pl.pallas_call(
            functools.partial(
                attend_kernel, base=chunk * part, part=part, span=span, head_dim=head_dim),
            grid=(owners // owner_group,),
            in_specs=[
                smem,
                pl.BlockSpec((owner_group, part * span, width), lambda i: (i, 0, 0)),
                pl.BlockSpec((held, length, width), lambda i: (0, 0, 0)),
                pl.BlockSpec((held, width, length), lambda i: (0, 0, 0)),
            ],
            out_specs=pl.BlockSpec((owner_group, back_rows, width), lambda i: (i, 0, 0)),
            out_shape=jax.ShapeDtypeStruct((owners, back_rows, width), bf16),
            compiler_params=params(("arbitrary",)),
        )(local, received[chunk], keys, values)
        back.append(lax.all_to_all(partial, "st", split_axis=0, concat_axis=0, tiled=True))

    half = jax.ShapeDtypeStruct((row_count // cores, width), bf16)
    keep, send = pl.pallas_call(
        functools.partial(
            merge_kernel,
            chunk_count=chunk_count,
            capacity=capacity,
            picks=picks,
            span=span,
            head_dim=head_dim,
        ),
        in_specs=[smem, smem, whole, whole] + [whole] * chunk_count,
        out_specs=[whole, whole],
        out_shape=[half, half],
        compiler_params=params(),
        name="merge",
    )(place, core, gated, gate, *back)
    other = lax.ppermute(send, "tp", [(0, 1), (1, 0)])
    column = model // 4
    return pl.pallas_call(
        output_kernel,
        grid=(4,),
        in_specs=[
            smem,
            pl.BlockSpec(half.shape, lambda i: (0, 0)),
            pl.BlockSpec(half.shape, lambda i: (0, 0)),
            pl.BlockSpec((width * cores, column), lambda i: (0, i)),
        ],
        out_specs=pl.BlockSpec((row_count // cores, column), lambda i: (0, i)),
        out_shape=jax.ShapeDtypeStruct((row_count // cores, model), bf16),
        compiler_params=params(("arbitrary",)),
        name="project",
    )(core, keep, other, output_weight)


def solution(mesh):
    in_specs = (
        P("st", None),
        P("st", None),
        P("st", None, None),
        P(),
        P(),
        P(None, "tp"),
        P(None, "tp"),
        P("tp"),
        P("tp", None, None),
        P("tp", None),
        P(None, "tp"),
        P(None, "tp"),
        P(None, "tp"),
        P(None, "tp"),
        P(),
    )
    out_specs = P(("st", "tp"), None)

    return jax.shard_map(
        per_device, mesh=mesh, in_specs=in_specs, out_specs=out_specs, check_vma=False
    )
```
